32 devices in a mesh: sp: 8 (over z, y), tp: 4 (over x, core).
Axes of the slice: x: 2, y: 2, z: 4, core: 2. Of those that a mesh axis runs over, the one named last changes fastest.
Arguments:
- tokens: bfloat16 [4096, 2048], P('sp'), may hold values from -6 to 6
- norm_gain: float32 [2048], replicated, may hold values from 0.1 to 1.9
- w_value: bfloat16 [2048, 512], P('sp', 'tp'), may hold values from -0.125 to 0.125
- w_gate: bfloat16 [2048, 512], P('sp', 'tp'), may hold values from -0.125 to 0.125
- w_drive: bfloat16 [2048, 512], P('sp', 'tp'), may hold values from -0.125 to 0.125
- conv_taps: float32 [31, 512], P(None, 'tp'), may hold values from -12 to 12
- conv_gain: float32 [512], P('tp'), may hold values from 0.1 to 1.9
- log_step: float32 [32], P('tp'), may hold values from -20 to -3
- step_shift: float32 [4096, 32], P('sp', 'tp'), may hold values from -1.5 to 12
- state_real: float32 [32, 64], P('tp'), may hold values from -1.2 to -0.5
- state_imag: float32 [32, 64], P('tp'), may hold values from 0 to 201.06177
- in_map: float32 [2, 32, 64, 16], P(None, 'tp'), may hold values from -6 to 6
- out_map: float32 [2, 32, 16, 64], P(None, 'tp'), may hold values from -1.5 to 1.5
- skip_gain: float32 [32, 16], P('tp'), may hold values from -3 to 3
- start_state: float32 [2, 32, 64], P(None, 'tp'), may hold values from -6 to 6
- conv_proj: bfloat16 [512, 2048], P('tp', 'sp'), may hold values from -0.1875 to 0.1875
- state_proj: bfloat16 [512, 2048], P('tp', 'sp'), may hold values from -0.1875 to 0.1875
Outputs:
- mixed: bfloat16 [4096, 2048], P('sp', 'tp')
The draws below stay inside these ranges and needn't reach their ends.
All inputs are finite; a program needn't handle non-finite values.
Results may differ from the reference program's by a relative error of at most 0.013.
Values may be sent and summed in bfloat16 or wider, within the bound.
No kernel may reach another device: no remote copies, remote signals or barrier semaphores. Data moves between devices by JAX's collectives and lax.ppermute only.
A program may use at most 64 MiB of HBM per device.

```python
import math
import jax
import jax.numpy as jnp
from jax import lax

D = 2048
CONV = 512
SSM = 512
GROUP = 16
STATE = 64
TAPS = 31
TOK_DEV = 512
GROUP_TOTAL = 32
TOKEN_LENGTH = 4096


def draw_conv_taps(key, part):
    first_key, second_key = jax.random.split(key)
    top_scale = 4.0
    rising = jnp.exp(math.log(top_scale) * jnp.arange(CONV, dtype=jnp.float32) / (CONV - 1))
    jitter = jnp.exp(jax.random.uniform(second_key, (CONV,), jnp.float32, -0.7, 0.7))
    normal_base = jnp.clip(jax.random.normal(first_key, (TAPS, CONV), jnp.float32), -4.0, 4.0)
    return normal_base * (rising * jitter / math.sqrt(TAPS))[None, :]


def draw_log_step(key, part):
    pick_key, jitter_key = jax.random.split(key)
    fast_share = 0.5
    fast_group = jax.random.bernoulli(pick_key, fast_share, (GROUP_TOTAL,))
    jitter = jax.random.uniform(jitter_key, (GROUP_TOTAL,), jnp.float32, -0.3, 0.3)
    slow_level = math.log(0.25 / TOKEN_LENGTH)
    fast_level = math.log(1.0 / 40.0)
    return jnp.where(fast_group, fast_level, slow_level) + jitter


def draw_step_shift(key, part):
    amplitude_key, coarse_key, location_key, spike_key = jax.random.split(key, 4)
    reach = 0.69
    block_count = TOKEN_LENGTH // TOK_DEV
    level = jax.random.uniform(amplitude_key, (block_count, 1, GROUP_TOTAL), jnp.float32, -reach, reach)
    rough = jax.random.uniform(coarse_key, (block_count, TOK_DEV, GROUP_TOTAL), jnp.float32, -0.35, 0.35)
    baseline_shift = (level + rough).reshape(TOKEN_LENGTH, GROUP_TOTAL)
    places = jax.random.randint(location_key, (3, GROUP_TOTAL), 0, TOKEN_LENGTH)
    spike_positions = jnp.any(jnp.arange(TOKEN_LENGTH)[:, None, None] == places[None], axis=1)
    spike_shift = math.log(1.5 * TOKEN_LENGTH) + jax.random.uniform(spike_key, (TOKEN_LENGTH, GROUP_TOTAL), jnp.float32, -0.3, 0.3)
    return jnp.where(spike_positions, spike_shift, baseline_shift)


def levels(stream_key, dims, cuts, low, high):
    def one(axis_at, shards_of):
        heights = jax.random.uniform(jax.random.fold_in(jax.random.fold_in(stream_key, 6), axis_at), (shards_of,), jnp.float32, low / len(cuts), high / len(cuts))
        return jnp.repeat(jnp.exp(heights), dims[axis_at] // shards_of).reshape((-1,) + (1,) * (len(dims) - axis_at - 1))

    level = one(*cuts[0])
    for cut in cuts[1:]:
        level = level * one(*cut)
    return level


def normal_values(rng, shape, scale, most, shards=(), kind=jnp.bfloat16):
    loudness = levels(rng, shape, shards, -0.22, 0.18) if shards else 1.0
    result = jax.random.normal(rng, shape, jnp.float32) * scale * loudness
    return jnp.minimum(jnp.maximum(result, -most), most).astype(kind)


def setup_inputs(seed: int = 0) -> dict:
    key_list = jax.random.split(jax.random.key(seed), 18)
    tokens = normal_values(key_list[0], (TOKEN_LENGTH, D), 1.0, 6.0, ((0, 8),))
    norm_gain = jnp.clip(1.0 + 0.18 * jax.random.normal(key_list[1], (D,), jnp.float32), 0.1, 1.9)
    w_value = normal_values(key_list[2], (D, CONV), D ** -0.5, 0.125, ((0, 8), (1, 4)))
    w_gate = normal_values(key_list[3], (D, CONV), D ** -0.5, 0.125, ((0, 8), (1, 4)))
    w_drive = normal_values(key_list[4], (D, SSM), D ** -0.5, 0.125, ((0, 8), (1, 4)))
    conv_taps = draw_conv_taps(jax.random.fold_in(key_list[17], 71), 0)
    conv_gain = jnp.clip(1.0 + 0.18 * jax.random.normal(key_list[6], (CONV,), jnp.float32), 0.1, 1.9)
    log_step = draw_log_step(jax.random.fold_in(key_list[17], 71), 0)
    step_shift = draw_step_shift(jax.random.fold_in(key_list[17], 71), 0)
    state_real = jnp.clip(-1.2 + 0.70000005 * jax.random.uniform(key_list[9], (GROUP_TOTAL, STATE), jnp.float32) ** levels(key_list[9], (GROUP_TOTAL, STATE), ((0, 4),), -0.2, 0.2), -1.2, -0.5)
    state_imag = jnp.clip(201.06177 * jax.random.uniform(key_list[10], (GROUP_TOTAL, STATE), jnp.float32) ** levels(key_list[10], (GROUP_TOTAL, STATE), ((0, 4),), -0.2, 0.2), 0.0, 201.06177)
    in_map = normal_values(key_list[11], (2, GROUP_TOTAL, STATE, GROUP), 1.0, 6.0, ((1, 4),), jnp.float32)
    out_map = normal_values(key_list[12], (2, GROUP_TOTAL, GROUP, STATE), 0.25, 1.5, ((1, 4),), jnp.float32)
    skip_gain = normal_values(key_list[13], (GROUP_TOTAL, GROUP), 0.5, 3.0, ((0, 4),), jnp.float32)
    start_state = normal_values(key_list[14], (2, GROUP_TOTAL, STATE), 1.0, 6.0, ((1, 4),), jnp.float32)
    conv_proj = normal_values(key_list[15], (CONV, D), (CONV + SSM) ** -0.5, 0.1875, ((0, 4), (1, 8)))
    state_proj = normal_values(key_list[16], (SSM, D), (CONV + SSM) ** -0.5, 0.1875, ((0, 4), (1, 8)))
    return dict(tokens=tokens, norm_gain=norm_gain, w_value=w_value, w_gate=w_gate, w_drive=w_drive, conv_taps=conv_taps, conv_gain=conv_gain, log_step=log_step, step_shift=step_shift, state_real=state_real, state_imag=state_imag, in_map=in_map, out_map=out_map, skip_gain=skip_gain, start_state=start_state, conv_proj=conv_proj, state_proj=state_proj)


def pair_combine(earlier, later):
    return (later[0] * earlier[0] - later[1] * earlier[1], later[0] * earlier[1] + later[1] * earlier[0], later[0] * earlier[2] - later[1] * earlier[3] + later[2], later[0] * earlier[3] + later[1] * earlier[2] + later[3])

def reference(tokens, norm_gain, w_value, w_gate, w_drive, conv_taps, conv_gain, log_step, step_shift, state_real, state_imag, in_map, out_map, skip_gain, start_state, conv_proj, state_proj):
    tokens_wide = tokens.astype(jnp.float32)
    inverse_rms = lax.rsqrt(lax.optimization_barrier(jnp.mean(tokens_wide * tokens_wide, axis=1, keepdims=True)) + 1e-06)
    normed = (tokens_wide * inverse_rms * norm_gain).astype(jnp.bfloat16)
    glu_value = jnp.dot(normed, w_value, preferred_element_type=jnp.float32).astype(jnp.bfloat16)
    glu_gate = jnp.dot(normed, w_gate, preferred_element_type=jnp.float32).astype(jnp.bfloat16)
    drive_in = jnp.dot(normed, w_drive, preferred_element_type=jnp.float32).astype(jnp.bfloat16)
    gated = (glu_value.astype(jnp.float32) * jax.nn.sigmoid(glu_gate.astype(jnp.float32))).astype(jnp.bfloat16)
    padded = jnp.concatenate([jnp.zeros((TAPS - 1, CONV), jnp.bfloat16), gated], axis=0)
    conv_mix = jnp.zeros((TOKEN_LENGTH, CONV), jnp.float32)
    for lag_index in range(TAPS):
        conv_mix = conv_mix + conv_taps[lag_index] * padded[lag_index:lag_index + TOKEN_LENGTH].astype(jnp.float32)
    row_mean = lax.optimization_barrier(jnp.mean(conv_mix, axis=1, keepdims=True))
    row_var = lax.optimization_barrier(jnp.mean(conv_mix * conv_mix, axis=1, keepdims=True)) - row_mean * row_mean
    conv_out = jax.nn.silu((conv_mix - row_mean) * lax.rsqrt(row_var + 1e-05) * conv_gain).astype(jnp.bfloat16)
    rate_re = state_real[None]
    rate_im = state_imag[None]
    rate_size = rate_re * rate_re + rate_im * rate_im
    block_count = TOKEN_LENGTH // TOK_DEV
    drive_blocks = drive_in.reshape(block_count, TOK_DEV, GROUP_TOTAL, GROUP)
    shift_blocks = step_shift.reshape(block_count, TOK_DEV, GROUP_TOTAL)

    def sweep(state_carry, inputs):
        carry_re, carry_im = state_carry
        drive_block, shift_block = inputs
        drive_wide = drive_block.astype(jnp.float32)
        step_full = jnp.exp(log_step[None, :] + shift_block)[:, :, None]
        decay_mag = jnp.exp(rate_re * step_full)
        keep_re = decay_mag * jnp.cos(rate_im * step_full)
        keep_im = decay_mag * jnp.sin(rate_im * step_full)
        mapped_re = jnp.einsum('tgh,gph->tgp', drive_wide, in_map[0], precision=lax.Precision.HIGHEST)
        mapped_im = jnp.einsum('tgh,gph->tgp', drive_wide, in_map[1], precision=lax.Precision.HIGHEST)
        minus_re = keep_re - 1.0
        coeff_re = (minus_re * rate_re + keep_im * rate_im) / rate_size
        coeff_im = (keep_im * rate_re - minus_re * rate_im) / rate_size
        input_re = coeff_re * mapped_re - coeff_im * mapped_im
        input_im = coeff_re * mapped_im + coeff_im * mapped_re
        cum_re, cum_im, local_re, local_im = lax.associative_scan(pair_combine, (keep_re, keep_im, input_re, input_im), axis=0)
        state_re = local_re + cum_re * carry_re[None] - cum_im * carry_im[None]
        state_im = local_im + cum_re * carry_im[None] + cum_im * carry_re[None]
        ssm_pre = jnp.einsum('tgp,ghp->tgh', state_re, out_map[0], precision=lax.Precision.HIGHEST) - jnp.einsum('tgp,ghp->tgh', state_im, out_map[1], precision=lax.Precision.HIGHEST) + skip_gain * drive_wide
        block_out = jax.nn.gelu(ssm_pre).reshape(TOK_DEV, SSM).astype(jnp.bfloat16)
        return ((state_re[-1], state_im[-1]), block_out)
    carried, ssm_blocks = lax.scan(sweep, (start_state[0], start_state[1]), (drive_blocks, shift_blocks))
    ssm_out = ssm_blocks.reshape(TOKEN_LENGTH, SSM)
    mixed = jnp.dot(conv_out, conv_proj, preferred_element_type=jnp.float32) + jnp.dot(ssm_out, state_proj, preferred_element_type=jnp.float32)
    return mixed.astype(jnp.bfloat16)
```

```python
import functools
import math

import jax
import jax.numpy as jnp
from jax import lax
from jax.experimental import pallas as pl
from jax.experimental.pallas import tpu as pltpu
from jax.sharding import PartitionSpec as P

F32 = jnp.float32
BF16 = jnp.bfloat16
HIGH = lax.Precision.HIGHEST
LANES = 128
CHUNKS = 8


SIN_TERMS = [(-1.0) ** n * math.pi ** (2 * n + 1) / math.factorial(2 * n + 1) for n in range(6)]
COS_TERMS = [(-1.0) ** n * math.pi ** (2 * n) / math.factorial(2 * n) for n in range(7)]


def polynomial(x, terms):
    total = jnp.full_like(x, terms[-1])
    for term in terms[-2::-1]:
        total = total * x + term
    return total


def dot(a, b, **extra):
    return jnp.dot(a, b, preferred_element_type=F32, **extra)


def call(body, outs, scalars, arrays, scratch=(), flops=0, name=None):
    vmem = pl.BlockSpec(memory_space=pltpu.VMEM)
    smem = pl.BlockSpec(memory_space=pltpu.SMEM)
    return pl.pallas_call(
        body,
        out_shape=[jax.ShapeDtypeStruct(shape, kind) for shape, kind in outs],
        in_specs=[smem] * len(scalars) + [vmem] * len(arrays),
        out_specs=[vmem] * len(outs),
        scratch_shapes=[pltpu.VMEM(shape, kind) for shape, kind in scratch],
        compiler_params=pltpu.CompilerParams(vmem_limit_bytes=48 * 1024 * 1024),
        cost_estimate=pl.CostEstimate(flops=flops, bytes_accessed=0, transcendentals=0),
        name=name,
    )(*scalars, *arrays)


def chunk_order(rows, forward):
    steps = rows // CHUNKS
    to = lax.broadcasted_iota(jnp.int32, (rows, rows), 0)
    source = lax.broadcasted_iota(jnp.int32, (rows, rows), 1)
    if forward:
        wanted = (to % CHUNKS) * steps + to // CHUNKS
    else:
        wanted = (to % steps) * CHUNKS + to // steps
    return (source == wanted).astype(F32).astype(BF16)


def norm_body(tokens, gain, out, plain):
    rows, width = tokens.shape
    block = 32

    def one(index, _):
        at = pl.ds(pl.multiple_of(index * block, block), block)
        wide = tokens[at, :].astype(F32)
        scale = lax.rsqrt(jnp.mean(wide * wide, axis=1, keepdims=True) + 1e-06)
        plain[at, :] = (wide * scale * gain[...]).astype(BF16)
        return 0

    lax.fori_loop(0, rows // block, one, 0)
    order = chunk_order(rows, True)
    part = math.gcd(width, 512)
    for index in range(width // part):
        at = slice(index * part, (index + 1) * part)
        out[:, at] = dot(order, plain[:, at]).astype(BF16)


def factor_body(shift, log_step, spread, rates, keep, coeff, cum, ends, prefix, steps_full):
    flat = rates.shape[1]
    steps = jnp.exp(shift[...] + log_step[...])
    steps_full[...] = dot(steps, spread[...], precision=HIGH)
    rate_re, rate_turn, inv_re, inv_im = (rates[n : n + 1, :] for n in range(4))
    expm1_terms = [1.0 / math.factorial(n + 1) for n in range(8)]

    def one(index, carry):
        cum_re, cum_im = carry
        at = pl.ds(pl.multiple_of(index * CHUNKS, CHUNKS), CHUNKS)
        step = steps_full[at, :]
        power = rate_re * step
        mag = jnp.exp(power)
        mag_less = jnp.where(power > -0.5, power * polynomial(jnp.maximum(power, -0.5), expm1_terms), mag - 1.0)
        turn = rate_turn * step
        turn = turn - jnp.floor(turn + 0.5)
        square = turn * turn
        half_sin = turn * polynomial(square, SIN_TERMS)
        half_cos = polynomial(square, COS_TERMS)
        cos_less = -2.0 * half_sin * half_sin
        cos = 1.0 + cos_less
        keep_re = mag * cos
        keep_im = mag * (2.0 * half_sin * half_cos)
        minus_re = mag_less * cos + cos_less
        keep[0, at, :] = keep_re
        keep[1, at, :] = keep_im
        coeff[0, at, :] = minus_re * inv_re + keep_im * inv_im
        coeff[1, at, :] = keep_im * inv_re - minus_re * inv_im
        new_re = keep_re * cum_re - keep_im * cum_im
        new_im = keep_re * cum_im + keep_im * cum_re
        cum[0, at, :] = new_re
        cum[1, at, :] = new_im
        return new_re, new_im

    one_re = jnp.ones((CHUNKS, flat), F32)
    end_re, end_im = lax.fori_loop(
        0, steps_full.shape[0] // CHUNKS, one, (one_re, jnp.zeros((CHUNKS, flat), F32)), unroll=2
    )
    ends[0] = end_re
    ends[1] = end_im
    run_re, run_im = one_re[:1], jnp.zeros((1, flat), F32)
    for chunk in range(CHUNKS):
        prefix[0, chunk : chunk + 1, :] = run_re
        prefix[1, chunk : chunk + 1, :] = run_im
        last_re, last_im = end_re[chunk : chunk + 1], end_im[chunk : chunk + 1]
        run_re, run_im = run_re * last_re - run_im * last_im, run_re * last_im + run_im * last_re
    prefix[0, CHUNKS : CHUNKS + 1, :] = run_re
    prefix[1, CHUNKS : CHUNKS + 1, :] = run_im


def project(normed, blocks, sources, width):
    total = jnp.zeros((normed.shape[0], width), F32)
    for block, source in zip(blocks, sources):
        rows = block.shape[0]
        at = pl.ds(pl.multiple_of(source * rows, rows), rows)
        total = total + dot(normed[:, at], block[...])
    return total


def scan_body(sources_of, counts, here, normed, *refs):
    blocks, refs = refs[: len(counts)], refs[len(counts) :]
    (in_mat, keep, coeff, ends, prefix, out_mat, skip, local_out, carries, message, mapped, states) = refs
    views = []
    for ref, count in zip(blocks, counts):
        views += [ref] if count is None else [ref.at[n] for n in range(count)]
    rows = normed.shape[0]
    flat = keep.shape[2]
    drive_wide = project(normed, views, sources_of(here[0]), local_out.shape[1])
    drive = drive_wide.astype(BF16)
    mapped[...] = dot(jnp.concatenate([drive, drive], axis=1), in_mat[...])

    def advance(at, carry):
        re, im = carry
        keep_re, keep_im = keep[0, at, :], keep[1, at, :]
        coeff_re, coeff_im = coeff[0, at, :], coeff[1, at, :]
        map_re, map_im = mapped[at, :flat], mapped[at, flat:]
        new_re = keep_re * re - keep_im * im + (coeff_re * map_re - coeff_im * map_im)
        new_im = keep_re * im + keep_im * re + (coeff_re * map_im + coeff_im * map_re)
        return new_re, new_im

    def one(index, carry):
        base = pl.multiple_of(index * 2 * CHUNKS, 2 * CHUNKS)
        first = advance(pl.ds(base, CHUNKS), carry)
        second = advance(pl.ds(base + CHUNKS, CHUNKS), first)
        at = pl.ds(base, 2 * CHUNKS)
        states[at, :flat] = jnp.concatenate([first[0], second[0]], axis=0).astype(BF16)
        states[at, flat:] = jnp.concatenate([first[1], second[1]], axis=0).astype(BF16)
        return second

    zero = jnp.zeros((CHUNKS, flat), F32)
    last_re, last_im = lax.fori_loop(0, rows // (2 * CHUNKS), one, (zero, zero), unroll=2)
    both = dot(states[...], out_mat[...])
    width = local_out.shape[1]
    local_out[...] = both[:, :width] + both[:, width:] + skip[...] * drive.astype(F32)
    run_re, run_im = zero[:1], zero[:1]
    end_re, end_im = ends[0], ends[1]
    for chunk in range(CHUNKS):
        carries[0, chunk : chunk + 1, :] = run_re
        carries[1, chunk : chunk + 1, :] = run_im
        at = slice(chunk, chunk + 1)
        run_re, run_im = (
            end_re[at] * run_re - end_im[at] * run_im + last_re[at],
            end_re[at] * run_im + end_im[at] * run_re + last_im[at],
        )
    message[0:1, :] = prefix[0, CHUNKS : CHUNKS + 1, :]
    message[1:2, :] = prefix[1, CHUNKS : CHUNKS + 1, :]
    message[2:3, :] = run_re
    message[3:4, :] = run_im


def join_rows(state, part):
    re, im = state
    return (
        part[0] * re - part[1] * im + part[2],
        part[0] * im + part[1] * re + part[3],
    )


def finish_body(entry_of, n_parts, here, *refs):
    parts, refs = refs[:n_parts], refs[n_parts:]
    start, cum, prefix, carries, local_out, out_mat, out, scaled = refs
    rows = local_out.shape[0]
    flat = cum.shape[2]
    entry_re, entry_im = entry_of(here[0], parts, (start[0:1, :], start[1:2, :]))
    pre_re, pre_im = prefix[0, :CHUNKS, :], prefix[1, :CHUNKS, :]
    carry_re = pre_re * entry_re - pre_im * entry_im + carries[0]
    carry_im = pre_re * entry_im + pre_im * entry_re + carries[1]

    def one(index, _):
        base = pl.multiple_of(index * 2 * CHUNKS, 2 * CHUNKS)
        made = []
        for half in range(2):
            at = pl.ds(base + half * CHUNKS, CHUNKS)
            cum_re, cum_im = cum[0, at, :], cum[1, at, :]
            made.append((cum_re * carry_re - cum_im * carry_im, cum_re * carry_im + cum_im * carry_re))
        at = pl.ds(base, 2 * CHUNKS)
        scaled[at, :flat] = jnp.concatenate([made[0][0], made[1][0]], axis=0).astype(BF16)
        scaled[at, flat:] = jnp.concatenate([made[0][1], made[1][1]], axis=0).astype(BF16)
        return 0

    lax.fori_loop(0, rows // (2 * CHUNKS), one, 0, unroll=2)
    both = dot(scaled[...], out_mat[...])
    width = local_out.shape[1]
    pre = both[:, :width] + both[:, width:] + local_out[...]
    done = jax.nn.gelu(pre).astype(BF16)
    out[...] = dot(chunk_order(rows, False), done).astype(BF16)


def gate_body(sources_of, counts, here, normed, *refs):
    blocks, (gated, tail) = refs[: len(counts)], refs[len(counts) :]
    views = []
    for ref, count in zip(blocks, counts):
        views += [ref] if count is None else [ref.at[n] for n in range(count)]
    width = gated.shape[1]
    total = project(normed, views, sources_of(here[0]), 2 * width)
    value = total[:, :width].astype(BF16).astype(F32)
    gate = total[:, width:].astype(BF16).astype(F32)
    gated[...] = (value * jax.nn.sigmoid(gate)).astype(BF16).astype(F32)
    reach = tail.shape[0]
    first = gated.shape[0] - reach * CHUNKS + CHUNKS - 1
    tail[...] = gated[pl.ds(first, reach, stride=CHUNKS), :].astype(BF16)


def conv_body(gated, halo, taps, gain, out, extended, mixed):
    rows, width = gated.shape
    steps = rows // CHUNKS
    tap_count = taps.shape[0]
    reach = tap_count - 1
    lane = lax.broadcasted_iota(jnp.int32, (CHUNKS, width), 0)
    before = halo[...].astype(F32)
    for lag in range(reach):
        tile = gated[(steps - reach + lag) * CHUNKS : (steps - reach + lag + 1) * CHUNKS, :]
        moved = pltpu.roll(tile, 1, 0)
        extended[lag * CHUNKS : (lag + 1) * CHUNKS, :] = jnp.where(lane == 0, before[lag : lag + 1, :], moved)
    extended[reach * CHUNKS :, :] = gated[...]
    group = math.gcd(steps, 8)

    def one(index, _):
        base = index * group * CHUNKS
        totals = [jnp.zeros((CHUNKS, width), F32) for _ in range(group)]
        for lag in range(tap_count + group - 1):
            at = pl.multiple_of(base + lag * CHUNKS, CHUNKS)
            tile = extended[pl.ds(at, CHUNKS), :]
            for n in range(group):
                if 0 <= lag - n < tap_count:
                    totals[n] = totals[n] + taps[lag - n : lag - n + 1, :] * tile
        for n in range(group):
            at = pl.multiple_of(base + n * CHUNKS, CHUNKS)
            mixed[pl.ds(at, CHUNKS), :] = totals[n]
        return 0

    lax.fori_loop(0, steps // group, one, 0)
    mix = mixed[...]
    ones = jnp.ones((CHUNKS, width), F32)
    sums = lax.dot_general(ones, mix, (((1,), (1,)), ((), ())), precision=HIGH, preferred_element_type=F32)
    mean = sums[:1, :] * (1.0 / width)

    def three(values):
        high = values.astype(BF16)
        rest = values - high.astype(F32)
        middle = rest.astype(BF16)
        return high.astype(F32), middle.astype(F32), (rest - middle.astype(F32))

    pieces = three(mean)
    column = spread_rows(pieces, rows, width)
    out[:rows, :] = (mix - column).astype(BF16)
    per = rows // LANES
    lines = []
    for piece in pieces:
        lines += [piece[:, n * LANES : (n + 1) * LANES] for n in range(per)]
    lines += list(three(gain[...]))
    lines += [jnp.zeros((1, width), F32)] * (out.shape[0] - rows - len(lines))
    out[rows:, :] = jnp.concatenate(lines, axis=0).astype(BF16)


def spread_rows(pieces, rows, width):
    lines = jnp.concatenate(list(pieces) + [jnp.zeros((CHUNKS - len(pieces), rows), F32)], axis=0)
    return lax.dot_general(
        lines.astype(BF16),
        jnp.ones((CHUNKS, width), BF16),
        (((0,), (0,)), ((), ())),
        preferred_element_type=F32,
    )


def mix_body(members, weight_at, w_counts, where, *refs):
    arrived, refs = refs[: len(members)], refs[len(members) :]
    weights, (total, w_state, active, w_conv, values) = refs[: len(w_counts)], refs[len(w_counts) :]
    views = []
    for ref, count in zip(weights, w_counts):
        views += [ref] if count is None else [ref.at[n] for n in range(count)]
    rows = total.shape[0]
    width = w_conv.shape[0] // (len(arrived_views(arrived, members)))
    tiles = arrived_views(arrived, members)
    per = rows // LANES
    means, gains = [], []
    for view in tiles:
        lines = view[rows:, :].astype(F32)
        pieces = [
            jnp.concatenate([lines[p * per + n : p * per + n + 1, :] for n in range(per)], axis=1)
            for p in range(3)
        ]
        means.append(spread_rows(pieces, rows, width))
        gains.append(lines[3 * per : 3 * per + 1] + lines[3 * per + 1 : 3 * per + 2] + lines[3 * per + 2 : 3 * per + 3])
    row_mean = sum(means[1:], means[0]) * (1.0 / len(tiles))
    squares = jnp.zeros((rows, width), F32)
    for n, view in enumerate(tiles):
        centred = view[:rows, :].astype(F32) + (means[n] - row_mean)
        values[n] = centred
        squares = squares + centred * centred
    row_var = jnp.sum(squares, axis=1, keepdims=True) * (1.0 / (len(tiles) * width))
    scale = lax.rsqrt(row_var + 1e-05)
    slots = members_of(members, where[1])
    for n, slot in enumerate(slots):
        active[slot] = jax.nn.silu(values[n] * scale * gains[n]).astype(BF16)
    for view, (row_slot, column_slot) in zip(views, weight_at(where[0])):
        high = view.shape[0] // 2
        wide = view.shape[1]
        row_at = pl.ds(pl.multiple_of(row_slot * high, high), high)
        column_at = pl.ds(pl.multiple_of(column_slot * wide, wide), wide)
        w_conv[row_at, column_at] = view[:high, :]
        w_state[row_at, column_at] = view[high:, :]
    joined = jnp.concatenate([active[n] for n in range(len(tiles))], axis=1)
    ordered = dot(chunk_order(rows, False), joined).astype(BF16)
    total[...] = dot(ordered, w_conv[...])


def arrived_views(arrived, members):
    views = []
    for ref, group in zip(arrived, members):
        views += [ref] if len(group) == 1 else [ref.at[n] for n in range(len(group))]
    return views


def members_of(members, mine):
    return [mine ^ flip for group in members for flip in group]


def last_body(members, where, *refs):
    arrived, (total, w_state, out, active) = refs[: len(members)], refs[len(members) :]
    tiles = arrived_views(arrived, members)
    for view, slot in zip(tiles, members_of(members, where[1])):
        active[slot] = view[...]
    joined = jnp.concatenate([active[n] for n in range(len(tiles))], axis=1)
    out[...] = (total[...] + dot(joined, w_state[...])).astype(BF16)


def shift(x, axis, by, inner):
    size = lax.axis_size(axis)
    return lax.ppermute(x, axis, [(i, (i + by * inner) % size) for i in range(size)])


def flip(x, axis, bit):
    return lax.ppermute(x, axis, [(i, i ^ bit) for i in range(lax.axis_size(axis))])


def outer_first(x, axis):
    outer = lax.axis_size(axis) // 2
    mine = [x] + [shift(x, axis, k, 2) for k in range(1, outer)]
    other = flip(jnp.stack(mine), axis, 1)

    def sources(s):
        z, y = s // 2, s % 2
        zs = [(z - k + outer) % outer for k in range(outer)]
        return [zz * 2 + y for zz in zs] + [zz * 2 + 1 - y for zz in zs]

    return mine + [other], [None] * outer + [outer], sources


def inner_first(x, axis):
    outer = lax.axis_size(axis) // 2
    pair = jnp.stack([x, flip(x, axis, 1)])
    parts = [pair] + [shift(pair, axis, k, 2) for k in range(1, outer)]

    def sources(s):
        z, y = s // 2, s % 2
        found = []
        for k in range(outer):
            zz = (z - k + outer) % outer
            found += [zz * 2 + y, zz * 2 + 1 - y]
        return found

    return parts, [2] * outer, sources


def gather_plain(x, axis):
    return [lax.all_gather(x, axis, axis=0, tiled=True)], [None], lambda s: [0]


def gather_members(x, axis):
    size = lax.axis_size(axis)
    held, flips = x[None], [0]
    bit = size // 2
    arrays, members = [x], [(0,)]
    while bit:
        came = flip(held if len(flips) > 1 else x, axis, bit)
        if bit == size // 2:
            new = [bit]
        else:
            new = [f ^ bit for f in flips]
        arrays.append(came)
        members.append(tuple(new))
        flips = flips + new
        bit //= 2
        if bit:
            held = jnp.stack([x, came]) if len(flips) == 2 else jnp.concatenate([held, came], axis=0)
    return arrays, members


def on_device(
    tokens,
    norm_gain,
    w_value,
    w_gate,
    w_drive,
    conv_taps,
    conv_gain,
    log_step,
    step_shift,
    state_real,
    state_imag,
    in_map,
    out_map,
    skip_gain,
    start_state,
    conv_proj,
    state_proj,
):
    rows, width = tokens.shape
    sp_size, tp_size = lax.axis_size("sp"), lax.axis_size("tp")
    here = jnp.stack([lax.axis_index("sp"), lax.axis_index("tp")]).astype(jnp.int32)
    small = sp_size % 2 == 0 and sp_size <= 8

    value_gate = jnp.concatenate([w_value, w_gate], axis=1)
    if small:
        vg_parts, vg_counts, vg_sources = outer_first(value_gate, "sp")
        drive_parts, drive_counts, drive_sources = inner_first(w_drive, "sp")
    else:
        vg_parts, vg_counts, vg_sources = gather_plain(value_gate, "sp")
        drive_parts, drive_counts, drive_sources = gather_plain(w_drive, "sp")

    per = sp_size // tp_size
    out_block = jnp.concatenate([conv_proj, state_proj], axis=0)
    pairs = [
        (s * tp_size + t, ((s % per) * tp_size + t) * tp_size + s // per)
        for s in range(sp_size)
        for t in range(tp_size)
    ]
    out_block = lax.ppermute(out_block, ("sp", "tp"), pairs)
    if small:
        out_parts, out_counts, out_sources = outer_first(out_block, "sp")
    else:
        gathered = lax.all_gather(out_block, "sp")
        arranged = gathered.reshape(per, tp_size, 2, -1, out_block.shape[1]).transpose(2, 1, 3, 0, 4)
        out_parts = [arranged.reshape(2 * arranged.shape[1] * arranged.shape[2], -1)]
        out_counts, out_sources = [None], None

    group_count, state_count = state_real.shape
    group_width = in_map.shape[3]
    flat = group_count * state_count
    channels = group_count * group_width
    same = jnp.eye(group_count, dtype=F32)
    rate_re, rate_im = state_real.reshape(1, flat), state_imag.reshape(1, flat)
    rate_size = rate_re * rate_re + rate_im * rate_im
    rates = jnp.concatenate(
        [rate_re, rate_im * (0.5 / math.pi), rate_re / rate_size, rate_im / rate_size], axis=0
    )
    steps = rows // CHUNKS
    shift_order = step_shift.reshape(CHUNKS, steps, group_count).transpose(1, 0, 2).reshape(rows, group_count)
    spread = jnp.repeat(same, state_count, axis=1)

    def two(matrix):
        high = matrix.astype(BF16)
        return high, (matrix - high.astype(F32)).astype(BF16)

    in_mat = jnp.einsum("rgph,gk->ghrkp", in_map, same, precision=HIGH).reshape(channels, 2 * flat)
    in_mat = jnp.concatenate(two(in_mat), axis=0)
    signs = jnp.array([1.0, -1.0], F32)[:, None, None, None]
    out_mat = jnp.einsum("rghp,gk->rgpkh", out_map * signs, same, precision=HIGH).reshape(2 * flat, channels)
    out_mat = jnp.concatenate(two(out_mat), axis=1)
    skip_row = skip_gain.reshape(1, channels)

    (normed,) = call(
        norm_body,
        [((rows, width), BF16)],
        [],
        [tokens, norm_gain.reshape(1, width)],
        [((rows, width), BF16)],
        flops=10**9,
        name="norm",
    )
    whole = (2, rows, flat)
    keep, coeff, cum, ends, prefix = call(
        factor_body,
        [(whole, F32), (whole, F32), (whole, F32), ((2, CHUNKS, flat), F32), ((2, CHUNKS + 1, flat), F32)],
        [],
        [shift_order, log_step.reshape(1, group_count), spread, rates],
        [((rows, flat), F32)],
        flops=10**9,
        name="factors",
    )

    local_out, carries, message = call(
        functools.partial(scan_body, drive_sources, drive_counts),
        [((rows, channels), F32), ((2, CHUNKS, flat), F32), ((4, flat), F32)],
        [here],
        [normed, *drive_parts, in_mat, keep, coeff, ends, prefix, out_mat, skip_row],
        [((rows, 2 * flat), F32), ((rows, 2 * flat), BF16)],
        flops=10**9,
        name="scan",
    )

    if small:
        outer = sp_size // 2
        partner = lax.ppermute(message, "sp", [(i, i ^ 1) for i in range(sp_size)])
        odd = (lax.axis_index("sp") % 2 == 1)
        first = jnp.where(odd, partner, message)
        second = jnp.where(odd, message, partner)
        pair = jnp.concatenate(
            [
                first[0:1] * second[0:1] - first[1:2] * second[1:2],
                first[0:1] * second[1:2] + first[1:2] * second[0:1],
                second[0:1] * first[2:3] - second[1:2] * first[3:4] + second[2:3],
                second[0:1] * first[3:4] + second[1:2] * first[2:3] + second[3:4],
            ],
            axis=0,
        )
        entry_parts = [partner] + [
            lax.ppermute(pair, "sp", [(i, i + 2 * k) for i in range(sp_size) if i + 2 * k < sp_size])
            for k in range(1, outer)
        ]

        def entry_of(s, parts, state):
            z = s // 2
            for k in range(outer - 1, 0, -1):
                joined = join_rows(state, [parts[k][n : n + 1, :] for n in range(4)])
                state = tuple(jnp.where(z >= k, new, old) for new, old in zip(joined, state))
            joined = join_rows(state, [parts[0][n : n + 1, :] for n in range(4)])
            return tuple(jnp.where(s % 2 == 1, new, old) for new, old in zip(joined, state))

    else:
        entry_parts = [lax.all_gather(message, "sp")]

        def entry_of(s, parts, state):
            def one(position, state):
                part = parts[0][position]
                joined = join_rows(state, [part[n : n + 1, :] for n in range(4)])
                return tuple(jnp.where(position < s, new, old) for new, old in zip(joined, state))

            return lax.fori_loop(0, sp_size - 1, one, state)

    tap_count, conv_width = conv_taps.shape
    gated, tail = call(
        functools.partial(gate_body, vg_sources, vg_counts),
        [((rows, conv_width), F32), ((tap_count - 1, conv_width), BF16)],
        [here],
        [normed, *vg_parts],
        flops=10**9,
        name="gate",
    )
    halo = lax.ppermute(tail, "sp", [(i, i + 1) for i in range(sp_size - 1)])
    extra = -(-(3 * (rows // LANES) + 3) // 16) * 16
    (mixed,) = call(
        conv_body,
        [((rows + extra, conv_width), BF16)],
        [],
        [gated, halo, conv_taps, conv_gain.reshape(1, conv_width)],
        [((rows + (tap_count - 1) * CHUNKS, conv_width), F32), ((rows, conv_width), F32)],
        flops=10**9,
        name="conv",
    )
    mix_arrays, members = gather_members(mixed, "tp")

    (state_out,) = call(
        functools.partial(finish_body, entry_of, len(entry_parts)),
        [((rows, channels), BF16)],
        [here],
        [*entry_parts, start_state.reshape(2, flat), cum, prefix, carries, local_out, out_mat],
        [((rows, 2 * flat), BF16)],
        flops=10**9,
        name="finish",
    )
    state_arrays, _ = gather_members(state_out, "tp")

    if small:

        def weight_at(s):
            return [(m % tp_size, m // tp_size) for m in out_sources(s)]

        wide = per * conv_proj.shape[1]
    else:

        def weight_at(s):
            return [(0, 0)]

        wide = per * conv_proj.shape[1]
    conv_all = conv_proj.shape[0] * tp_size
    total, w_state = call(
        functools.partial(mix_body, members, weight_at, out_counts),
        [((rows, wide), F32), ((conv_all, wide), BF16)],
        [here],
        [*mix_arrays, *out_parts],
        [
            ((tp_size, rows, conv_width), BF16),
            ((conv_all, wide), BF16),
            ((tp_size, rows, conv_width), F32),
        ],
        flops=10**9,
        name="mix",
    )
    (out,) = call(
        functools.partial(last_body, members),
        [((rows, wide), BF16)],
        [here],
        [*state_arrays, total, w_state],
        [((tp_size, rows, channels), BF16)],
        flops=10**9,
        name="last",
    )
    return out


def solution(mesh):
    return jax.shard_map(
        on_device,
        mesh=mesh,
        in_specs=(
            P("sp", None),
            P(),
            P("sp", "tp"),
            P("sp", "tp"),
            P("sp", "tp"),
            P(None, "tp"),
            P("tp"),
            P("tp"),
            P("sp", "tp"),
            P("tp", None),
            P("tp", None),
            P(None, "tp", None, None),
            P(None, "tp", None, None),
            P("tp", None),
            P(None, "tp", None),
            P("tp", "sp"),
            P("tp", "sp"),
        ),
        out_specs=P("sp", "tp"),
        check_vma=False,
    )
```
